32 devices in a mesh: ep: 8 (over z, x), tp: 4 (over y, core).
Axes of the slice: x: 2, y: 2, z: 4, core: 2. Of those that a mesh axis runs over, the one named last changes fastest.
Arguments:
- tokens: bfloat16 [1024, 4096], P('ep', 'tp'), may hold values from -16 to 16
- expert_ids: int32 [1024, 2], P('ep'), may hold values from 0 to 7, as said below
- group_weight: float32 [1024], P('ep'), may hold values from 0.25 to 1
- expert_weight: float32 [1024, 2], P('ep'), may hold values from 0.1 to 1
- w_gate: bfloat16 [8, 4096, 512], P('ep', None, 'tp'), may hold values from -0.09375 to 0.09375
- w_up: bfloat16 [8, 4096, 512], P('ep', None, 'tp'), may hold values from -0.09375 to 0.09375
- w_down: bfloat16 [8, 512, 4096], P('ep', None, 'tp'), may hold values from -0.5 to 0.5
- norm_gain: float32 [4096], P('tp'), may hold values from 0.1 to 1.9
- norm_bias: float32 [4096], P('tp'), may hold values from -3 to 3
Outputs:
- normed: bfloat16 [1024, 4096], P('ep', 'tp')
The draws below stay inside these ranges and needn't reach their ends.
Inputs may be any that keep to these rules, and one draw needn't show every extreme that they name: `expert_ids`: each row names 2 different experts of one group, a group being 2 consecutive ids; in the rows of one ep index each group is named by a 4-th of the rows. In the rows of one ep index no expert is named more than 32 times, and in every group one expert is named exactly 32 times in the rows of every ep index.
All inputs are finite; a program needn't handle non-finite values.
Results may differ from the reference program's by a relative error of at most 0.0045.
Values may be sent and summed in bfloat16 or wider, within the bound.
A program may use at most 64 MiB of HBM per device.

```python
import math
import jax
import jax.numpy as jnp
from jax import lax

D = 4096
FF = 512
GROUPS = 4
TOP_K = 2
TOK_DEV = 128
EXPERTS = 8
CAP = 32
TOKENS = 1024
N_EP = 8


def draw_tokens(key, part):
    quarter = (jnp.arange(D, dtype=jnp.int32) // (D // 4)).astype(jnp.float32)
    column_scale = 0.5 + 0.5 * quarter
    column_shift = 0.6 * (quarter - 1.5)
    values = jax.random.normal(jax.random.fold_in(key, 5), (TOKENS, D), jnp.float32)
    values = jnp.clip(values * column_scale[None, :] + column_shift[None, :], -16.0, 16.0)
    return values.astype(jnp.bfloat16)


def draw_expert_ids(key, part):
    per_group = EXPERTS // GROUPS
    pair_count = TOK_DEV // GROUPS
    block_count = TOKENS // TOK_DEV
    fixed_local = jax.random.randint(jax.random.fold_in(key, 1), (GROUPS,), 0, per_group)
    local_ids = jnp.arange(per_group, dtype=jnp.int32)
    pair_index = jnp.arange(pair_count, dtype=jnp.int32)
    first_rank = pair_index // CAP
    second_rank = (pair_index + pair_count) // CAP

    def one_block(index):
        block_key = jax.random.fold_in(key, index + 7)
        scores = jax.random.randint(jax.random.fold_in(block_key, 0), (GROUPS, per_group), 0, 1 << 20)
        scores = scores * per_group + local_ids[None, :]
        scores = jnp.where(local_ids[None, :] == fixed_local[:, None], -1, scores)
        order = jnp.argsort(scores, axis=1, stable=True).astype(jnp.int32)
        first = order[:, first_rank]
        second = order[:, second_rank]
        local_pair = jnp.stack([first, second], axis=-1)
        global_pair = local_pair + (jnp.arange(GROUPS, dtype=jnp.int32) * per_group)[:, None, None]
        flat_pairs = global_pair.reshape(TOK_DEV, 2)
        shuffle = jax.random.permutation(jax.random.fold_in(block_key, 1), TOK_DEV)
        return flat_pairs[shuffle]
    drawn = jax.vmap(one_block)(jnp.arange(block_count, dtype=jnp.int32))
    return drawn.reshape(TOKENS, 2).astype(jnp.int32)


def level_of(rng, extent, pieces, low, largest):
    factor_of, own = 1.0, jax.random.fold_in(rng, 6)
    for dim, shards_of in pieces:
        draws = jnp.exp(jax.random.uniform(jax.random.fold_in(own, dim), (shards_of,), jnp.float32, low / len(pieces), largest / len(pieces)))
        factor_of = factor_of * jnp.repeat(draws, extent[dim] // shards_of).reshape([-1 if axis == dim else 1 for axis in range(len(extent))])
    return factor_of


def noise(stream_key, shape, scale, reach, split=(), kind=jnp.bfloat16):
    gain = level_of(stream_key, shape, split, -0.22, 0.18) if split else 1.0
    values = jax.random.normal(stream_key, shape, jnp.float32) * scale * gain
    return jnp.minimum(jnp.maximum(values, -reach), reach).astype(kind)


def setup_inputs(seed: int = 0) -> dict:
    key_of = jax.random.split(jax.random.key(seed), 10)
    return {
        "tokens": draw_tokens(jax.random.fold_in(key_of[9], 71), 0),
        "expert_ids": draw_expert_ids(jax.random.fold_in(key_of[9], 71), 0),
        "group_weight": jnp.clip(jnp.exp(math.log(1.0) - 1.3862944 * jax.random.uniform(key_of[2], (TOKENS,), jnp.float32) ** level_of(key_of[2], (TOKENS,), ((0, 8),), -0.2, 0.2)), 0.25, 1.0),
        "expert_weight": jnp.clip(jnp.exp(math.log(1.0) - 2.3025851 * jax.random.uniform(key_of[3], (TOKENS, TOP_K), jnp.float32) ** level_of(key_of[3], (TOKENS, TOP_K), ((0, 8),), -0.2, 0.2)), 0.1, 1.0),
        "w_gate": noise(key_of[4], (EXPERTS, D, FF), D ** -0.5, 0.09375, ((0, 8), (2, 4))),
        "w_up": noise(key_of[5], (EXPERTS, D, FF), D ** -0.5, 0.09375, ((0, 8), (2, 4))),
        "w_down": noise(key_of[6], (EXPERTS, FF, D), (FF // 4) ** -0.5, 0.5, ((0, 8), (2, 4))),
        "norm_gain": jnp.clip(1.0 + 0.18 * jax.random.normal(key_of[7], (D,), jnp.float32), 0.1, 1.9),
        "norm_bias": noise(key_of[8], (D,), 0.5, 3.0, ((0, 4),), jnp.float32),
    }


residual_scale = 2.0 ** 0.5
norm_eps = 1e-05

def reference(tokens, expert_ids, group_weight, expert_weight, w_gate, w_up, w_down, norm_gain, norm_bias):
    block_count = TOKENS // TOK_DEV
    rows_per = N_EP * CAP
    flat_ids = expert_ids.reshape(block_count, TOK_DEV * TOP_K).astype(jnp.int32)
    one_hot = (flat_ids[:, :, None] == jnp.arange(EXPERTS, dtype=jnp.int32)[None, None, :]).astype(jnp.int32)
    prior_counts = jnp.cumsum(one_hot, axis=1) - one_hot
    slot_index = lax.optimization_barrier(jnp.sum(prior_counts * one_hot, axis=2)).astype(jnp.int32)
    block_start = (jnp.arange(block_count, dtype=jnp.int32) * CAP)[:, None]
    position = (flat_ids * rows_per + block_start + slot_index).reshape(-1).astype(jnp.int32)
    owner_token = (jnp.arange(TOKENS * TOP_K, dtype=jnp.int32) // TOP_K).astype(jnp.int32)
    slot_table = jnp.full((EXPERTS * rows_per,), TOKENS, jnp.int32).at[position].set(owner_token)
    padded = jnp.concatenate([tokens, jnp.zeros((1, D), tokens.dtype)], axis=0)

    def expert(inputs):
        table_rows, gate_w, up_w, down_w = inputs
        row_block = padded[table_rows]
        gate_sum = jnp.dot(row_block, gate_w, preferred_element_type=jnp.float32)
        up_sum = jnp.dot(row_block, up_w, preferred_element_type=jnp.float32)
        hidden = (jax.nn.silu(gate_sum) * up_sum).astype(jnp.bfloat16)
        return jnp.dot(hidden, down_w, preferred_element_type=jnp.float32).astype(jnp.bfloat16)
    results = lax.map(expert, (slot_table.reshape(EXPERTS, rows_per), w_gate, w_up, w_down))
    picked = results.reshape(EXPERTS * rows_per, D)[position].reshape(TOKENS, TOP_K, D).astype(jnp.float32)
    share_weight = group_weight[:, None] * expert_weight / lax.optimization_barrier(jnp.sum(expert_weight, axis=1, keepdims=True))
    routed = jnp.einsum('tk,tkd->td', share_weight.astype(jnp.float32), picked)
    mixed = residual_scale * tokens.astype(jnp.float32) + routed
    center = lax.optimization_barrier(jnp.mean(mixed, axis=1, keepdims=True))
    centered = mixed - center
    spread = lax.optimization_barrier(jnp.mean(centered * centered, axis=1, keepdims=True))
    normed = centered * lax.rsqrt(spread + norm_eps) * norm_gain[None, :] + norm_bias[None, :]
    return normed.astype(jnp.bfloat16)
```

```python
import functools

import jax
import jax.numpy as jnp
from jax import lax
from jax.experimental import pallas as pl
from jax.experimental.pallas import tpu as pltpu
from jax.sharding import PartitionSpec as P

D = 4096
GROUPS = 4
TOP_K = 2


residual_scale = 2.0**0.5
norm_eps = 1e-05


def on_device(
    tokens, expert_ids, group_weight, expert_weight, w_gate, w_up, w_down, norm_gain, norm_bias
):
    tok_count = tokens.shape[0]
    expert_count = lax.axis_size("ep")
    capacity = min(tok_count // GROUPS, 3 * TOP_K * tok_count // (2 * expert_count))
    pair_count = tok_count * TOP_K
    flat_ids = expert_ids.reshape(pair_count)
    one_hot = (flat_ids[:, None] == jnp.arange(expert_count, dtype=jnp.int32)[None, :]).astype(
        jnp.float32
    )
    earlier = (jnp.arange(pair_count)[:, None] > jnp.arange(pair_count)[None, :]).astype(
        jnp.float32
    )
    prior_counts = jnp.dot(
        earlier, one_hot, preferred_element_type=jnp.float32, precision=lax.Precision.HIGHEST
    )
    slot_index = jnp.sum(prior_counts * one_hot, axis=1).astype(jnp.int32)
    position = flat_ids * capacity + slot_index
    owner_token = jnp.arange(pair_count, dtype=jnp.int32) // TOP_K
    slot_table = (
        jnp.full((expert_count * capacity,), tok_count, jnp.int32).at[position].set(owner_token)
    )
    gate_local = w_gate[0]
    up_local = w_up[0]
    down_local = w_down[0]
    padded = jnp.concatenate([tokens, jnp.zeros((1, tokens.shape[1]), tokens.dtype)], axis=0)
    outgoing = padded[slot_table].reshape(expert_count, capacity, tokens.shape[1])
    arrived = lax.all_to_all(outgoing, "ep", split_axis=0, concat_axis=0, tiled=True)
    sources, slot_count, slice_width = arrived.shape
    row_block = arrived.reshape(sources * slot_count, slice_width)
    row_piece = lax.all_gather(row_block, "tp", axis=1, tiled=True)
    gate_sum = jnp.dot(row_piece, gate_local, preferred_element_type=jnp.float32)
    up_sum = jnp.dot(row_piece, up_local, preferred_element_type=jnp.float32)
    hidden = (jax.nn.silu(gate_sum) * up_sum).astype(jnp.bfloat16)
    result = jnp.dot(
        lax.all_gather(hidden, "tp", axis=1, tiled=True),
        down_local,
        preferred_element_type=jnp.float32,
    )
    result = result.astype(jnp.bfloat16).reshape(sources, slot_count, down_local.shape[1])
    returned = lax.all_to_all(result, "ep", split_axis=0, concat_axis=0, tiled=True)
    flat_rows = returned.reshape(expert_count * capacity, returned.shape[2])
    picked = flat_rows[position].reshape(tok_count, TOP_K, returned.shape[2]).astype(jnp.float32)
    share_weight = (
        group_weight[:, None] * expert_weight / jnp.sum(expert_weight, axis=1, keepdims=True)
    )
    routed = jnp.einsum("tk,tkd->td", share_weight, picked)
    mixed = residual_scale * tokens.astype(jnp.float32) + routed
    first_sum, second_sum = lax.psum((jnp.sum(mixed, axis=1), jnp.sum(mixed * mixed, axis=1)), "tp")
    center = first_sum / D
    spread = second_sum / D - center * center
    centered = mixed - center[:, None]
    normed = (
        centered * lax.rsqrt(spread + norm_eps)[:, None] * norm_gain[None, :] + norm_bias[None, :]
    )
    return normed.astype(jnp.bfloat16)


MESH = pl.DeviceIdType.MESH
F32 = jnp.float32
BF16 = jnp.bfloat16
(TO_PLANE, SHARES, CORE_OWN, ACROSS_X, ACROSS_Y, CORE_X, CORE_Y, RELAY_X, RELAY_Y,
 CORE_RX, CORE_RY, HIDDEN_0, HIDDEN_1, RESULT, BACK, STATS) = range(16)
KINDS = 16


def flip(value, bits):
    bit = 1
    while bit <= bits:
        if bits & bit:
            value = value + bit - 2 * bit * lax.rem(lax.div(value, bit), 2)
        bit *= 2
    return value


def layer_kernel(
    n_plane, n_tp,
    tokens_ref, ids_ref, group_ref, expert_ref, gate_hbm, up_hbm, down_hbm, gain_ref, bias_ref,
    out_ref,
    w_in, w_out, outgoing, share_out, share_in, rows, hidden, own_part, result_out, result_in,
    back_out, back_in, stats, send_sem, recv_sem, load_sem,
):
    ep = lax.axis_index("ep")
    q = lax.axis_index("tp")
    z, x = lax.div(ep, 2), lax.rem(ep, 2)
    ox = 1 - x
    q_core, q_y, q_diag = flip(q, 1), flip(q, 2), flip(q, 3)
    core_peer, y_peer, diag_peer = (ep, q_core), (ep, q_y), (ep, q_diag)
    x_peer = (z * 2 + ox, q)

    def plane_peer(d):
        return (flip(z, d) * 2 + x, q)

    tok, width = tokens_ref.shape
    cap = tok // n_plane
    half = cap // 2
    inner = gate_hbm.shape[2]

    barrier = pltpu.get_barrier_semaphore()
    partners = [plane_peer(d) for d in range(1, n_plane)] + [x_peer, core_peer, y_peer, diag_peer]
    for peer in partners:
        pl.semaphore_signal(barrier, inc=1, device_id=peer, device_id_type=MESH)

    loads = [
        pltpu.make_async_copy(gate_hbm.at[0], w_in.at[:, pl.ds(0, inner)], load_sem.at[0]),
        pltpu.make_async_copy(up_hbm.at[0], w_in.at[:, pl.ds(inner, inner)], load_sem.at[1]),
        pltpu.make_async_copy(down_hbm.at[0], w_out, load_sem.at[2]),
    ]
    for load in loads:
        load.start()

    first = ids_ref[0:1, :]
    group_row = (first >> 1).astype(F32)
    on_lanes = jnp.broadcast_to(group_row, (tok, tok))
    on_rows = jnp.transpose(on_lanes)
    ii = lax.broadcasted_iota(jnp.int32, (tok, tok), 0)
    jj = lax.broadcasted_iota(jnp.int32, (tok, tok), 1)
    same = on_lanes == on_rows
    zero, one = jnp.zeros((tok, tok), F32), jnp.ones((tok, tok), F32)
    rank_row = jnp.sum(jnp.where(same & (ii < jj), one, zero), axis=0, keepdims=True)
    rank_col = jnp.sum(jnp.where(same & (jj < ii), one, zero), axis=1, keepdims=True)
    place_row = group_row * cap + rank_row
    place_col = on_rows[:, 0:1] * cap + rank_col
    to_slot = jnp.broadcast_to(place_row, (tok, tok)) == ii.astype(F32)
    to_token = jnp.broadcast_to(place_col, (tok, tok)) == jj.astype(F32)

    sorted_rows = jnp.dot(
        jnp.where(to_slot, one, zero).astype(BF16), tokens_ref[...], preferred_element_type=F32
    ).astype(BF16)
    outgoing[...] = sorted_rows.reshape(n_plane, cap, width)
    rows[q, x, z] = outgoing[z]

    weights = expert_ref[...]
    share = group_ref[...] * weights / jnp.sum(weights, axis=0, keepdims=True)
    even = (first & 1) == 0
    share_a = jnp.where(even, share[0:1, :], share[1:2, :])
    share_b = jnp.where(even, share[1:2, :], share[0:1, :])
    slot_a = jnp.sum(jnp.where(to_slot, jnp.broadcast_to(share_a, (tok, tok)), zero), axis=1, keepdims=True)
    slot_b = jnp.sum(jnp.where(to_slot, jnp.broadcast_to(share_b, (tok, tok)), zero), axis=1, keepdims=True)
    lane = lax.broadcasted_iota(jnp.int32, (tok, 128), 1)
    share_out[...] = jnp.where(lane < 64, slot_a, slot_b).reshape(n_plane, cap, 128)
    share_in[z] = share_out[z]

    pl.semaphore_wait(barrier, len(partners))

    started = []

    def copy(src, dst, kind, j, peer):
        return pltpu.make_async_remote_copy(
            src_ref=src, dst_ref=dst, send_sem=send_sem.at[kind, j], recv_sem=recv_sem.at[kind, j],
            device_id=peer, device_id_type=MESH,
        )

    def send(src, dst, kind, j, peer):
        c = copy(src, dst, kind, j, peer)
        c.start()
        started.append(c)

    def arrived(dst, kind, j):
        copy(dst, dst, kind, j, core_peer).wait_recv()

    for d in range(1, n_plane):
        send(outgoing.at[flip(z, d)], rows.at[q, x, z], TO_PLANE, d, plane_peer(d))

    low, high = pl.ds(0, half), pl.ds(half, half)

    def spread_own(j):
        block = rows.at[q, x, flip(z, j)]
        if j:
            arrived(block, TO_PLANE, j)
        send(block, block, ACROSS_X, j, x_peer)
        send(block, block, ACROSS_Y, j, y_peer)
        send(block, block, CORE_OWN, j, core_peer)

    def pass_on(j):
        zz = flip(z, j)
        block = rows.at[q, ox, zz]
        arrived(block, ACROSS_X, j)
        send(block.at[low], block.at[low], RELAY_Y, j, y_peer)
        send(block, block, CORE_X, j, core_peer)
        block = rows.at[q_y, x, zz]
        arrived(block, ACROSS_Y, j)
        send(block.at[high], block.at[high], RELAY_X, j, x_peer)
        send(block, block, CORE_Y, j, core_peer)

    def pass_relayed(j):
        block = rows.at[q_y, ox, flip(z, j)]
        arrived(block.at[low], RELAY_Y, j)
        send(block.at[low], block.at[low], CORE_RY, j, core_peer)
        arrived(block.at[high], RELAY_X, j)
        send(block.at[high], block.at[high], CORE_RX, j, core_peer)

    for step in range(n_plane + 1):
        if step < n_plane:
            spread_own(step)
        if step == 0:
            for d in range(1, n_plane):
                send(share_out.at[flip(z, d)], share_in.at[z], SHARES, d, plane_peer(d))
        if step >= 1:
            pass_on(step - 1)
        if step >= 2:
            pass_relayed(step - 2)

    def sums_of(column, quarter):
        part = rows[quarter, column].reshape(tok, width)
        w = w_in[pl.ds(pl.multiple_of(quarter * width, width), width), :]
        return jnp.dot(part, w, preferred_element_type=F32)

    def finish_hidden(total, column, kind):
        gate, up = total[:, :inner], total[:, inner:]
        hidden[column, q] = (gate / (1.0 + jnp.exp(-gate)) * up).astype(BF16)
        block = hidden.at[column, q]
        for d, peer in ((2, y_peer), (3, diag_peer), (1, core_peer)):
            send(block, block, kind, d, peer)

    def project(column, kind):
        for d in range(1, n_tp):
            arrived(hidden.at[column, flip(q, d)], kind, d)
        h = jnp.concatenate([hidden[column, t] for t in range(n_tp)], axis=1)
        return jnp.dot(h, w_out[...], preferred_element_type=F32).astype(BF16)

    loads[0].wait()
    loads[1].wait()
    total = sums_of(x, q) + sums_of(x, q_y)
    other = sums_of(ox, q)
    for j in range(n_plane):
        arrived(rows.at[q_core, x, flip(z, j)], CORE_OWN, j)
        arrived(rows.at[q_diag, x, flip(z, j)], CORE_Y, j)
    total = total + sums_of(x, q_core) + sums_of(x, q_diag)
    finish_hidden(total, x, HIDDEN_0)
    pass_relayed(n_plane - 1)
    for j in range(n_plane):
        arrived(rows.at[q_core, ox, flip(z, j)], CORE_X, j)
    other = other + sums_of(ox, q_core) + sums_of(ox, q_y)
    for j in range(n_plane):
        block = rows.at[q_diag, ox, flip(z, j)]
        arrived(block.at[low], CORE_RY, j)
        arrived(block.at[high], CORE_RX, j)
    other = other + sums_of(ox, q_diag)
    finish_hidden(other, ox, HIDDEN_1)

    loads[2].wait()
    for d in range(1, n_plane):
        arrived(share_in.at[flip(z, d)], SHARES, d)
    shares = share_in[...].reshape(tok, 128)
    is_first = x == 0
    share_own = jnp.where(is_first, shares[:, 0:1], shares[:, 64:65])
    share_other = jnp.where(is_first, shares[:, 64:65], shares[:, 0:1])
    own_part[...] = (project(x, HIDDEN_0).astype(F32) * share_own).reshape(n_plane, cap, width)
    share_in[...] = jnp.broadcast_to(share_other, (tok, 128)).reshape(n_plane, cap, 128)

    result_out[...] = project(ox, HIDDEN_1).reshape(n_plane, cap, width)
    order = tuple(range(n_plane - 1, -1, -1))
    for j in order:
        zz = flip(z, j)
        send(result_out.at[zz], result_in.at[zz], RESULT, j, x_peer)
    for j in order:
        zz = flip(z, j)
        arrived(result_in.at[zz], RESULT, j)
        mixed_rows = own_part[zz] + result_in[zz].astype(F32) * share_in[zz][:, 0:1]
        if j:
            back_out[zz] = mixed_rows.astype(BF16)
            send(back_out.at[zz], back_in.at[z], BACK, j, plane_peer(j))
        else:
            back_in[z] = mixed_rows.astype(BF16)
    for j in order:
        if j:
            arrived(back_in.at[flip(z, j)], BACK, j)
    routed = jnp.dot(
        jnp.where(to_token, one, zero).astype(BF16),
        back_in[...].reshape(tok, width),
        preferred_element_type=F32,
    )
    mixed = residual_scale * tokens_ref[...].astype(F32) + routed
    total_col = jnp.sum(mixed, axis=1, keepdims=True)
    centered = mixed - total_col / width
    square_col = jnp.sum(centered * centered, axis=1, keepdims=True)
    lane = lax.broadcasted_iota(jnp.int32, (tok, 128), 1)
    stats[q] = jnp.transpose(jnp.where(lane == 0, total_col, square_col))[0:8, :]
    for d, peer in ((3, diag_peer), (2, y_peer), (1, core_peer)):
        send(stats.at[q], stats.at[q], STATS, d, peer)
    for d in range(1, n_tp):
        arrived(stats.at[flip(q, d)], STATS, d)
    pieces = [stats[t] for t in range(n_tp)]
    full = width * n_tp
    center = sum(p[0:1, :] for p in pieces) / full
    spread = sum(p[1:2, :] + width * jnp.square(p[0:1, :] / width - center) for p in pieces) / full
    scale = lax.rsqrt(spread + norm_eps)
    sub = lax.broadcasted_iota(jnp.int32, (128, tok), 0)
    columns = jnp.transpose(jnp.where(sub == 0, center, scale))
    out_ref[...] = (
        (mixed - columns[:, 0:1]) * columns[:, 1:2] * gain_ref[...] + bias_ref[...]
    ).astype(BF16)
    for c in started:
        c.wait_send()


def pair_groups(
    tokens, expert_ids, group_weight, expert_weight, w_gate, w_up, w_down, norm_gain, norm_bias
):
    tok, width = tokens.shape
    n_plane = lax.axis_size("ep") // TOP_K
    n_tp = lax.axis_size("tp")
    cap = tok // n_plane
    inner = w_gate.shape[2]
    vmem = pl.BlockSpec(memory_space=pltpu.VMEM)
    hbm = pl.BlockSpec(memory_space=pltpu.HBM)
    return pl.pallas_call(
        functools.partial(layer_kernel, n_plane, n_tp),
        out_shape=jax.ShapeDtypeStruct((tok, width), BF16),
        in_specs=[vmem, vmem, vmem, vmem, hbm, hbm, hbm, vmem, vmem],
        out_specs=vmem,
        scratch_shapes=[
            pltpu.VMEM((w_gate.shape[1], 2 * inner), BF16),
            pltpu.VMEM(w_down.shape[1:], BF16),
            pltpu.VMEM((n_plane, cap, width), BF16),
            pltpu.VMEM((n_plane, cap, 128), F32),
            pltpu.VMEM((n_plane, cap, 128), F32),
            pltpu.VMEM((n_tp, 2, n_plane, cap, width), BF16),
            pltpu.VMEM((2, n_tp, tok, inner), BF16),
            pltpu.VMEM((n_plane, cap, width), F32),
            pltpu.VMEM((n_plane, cap, width), BF16),
            pltpu.VMEM((n_plane, cap, width), BF16),
            pltpu.VMEM((n_plane, cap, width), BF16),
            pltpu.VMEM((n_plane, cap, width), BF16),
            pltpu.VMEM((n_tp, 8, tok), F32),
            pltpu.SemaphoreType.DMA((KINDS, 4)),
            pltpu.SemaphoreType.DMA((KINDS, 4)),
            pltpu.SemaphoreType.DMA((3,)),
        ],
        compiler_params=pltpu.CompilerParams(
            collective_id=0, has_side_effects=True, vmem_limit_bytes=56 * 2**20
        ),
        name="layer",
    )(
        tokens, expert_ids.T, group_weight[None, :], expert_weight.T, w_gate, w_up, w_down,
        norm_gain[None, :], norm_bias[None, :],
    )


def solution(mesh):
    n_ep, n_tp = mesh.shape["ep"], mesh.shape["tp"]
    pairs = TOP_K == 2 and n_ep == GROUPS * TOP_K and n_tp == 4
    return jax.shard_map(
        pair_groups if pairs else on_device,
        mesh=mesh,
        in_specs=(
            P("ep", "tp"),
            P("ep", None),
            P("ep"),
            P("ep", None),
            P("ep", None, "tp"),
            P("ep", None, "tp"),
            P("ep", None, "tp"),
            P("tp"),
            P("tp"),
        ),
        out_specs=P("ep", "tp"),
        check_vma=False,
    )
```

```python
import functools

import jax
import jax.numpy as jnp
from jax import lax
from jax.experimental import pallas as pl
from jax.experimental.pallas import tpu as pltpu
from jax.sharding import PartitionSpec as P

D = 4096
GROUPS = 4
TOP_K = 2


residual_scale = 2.0**0.5
norm_eps = 1e-05


def on_device(
    tokens, expert_ids, group_weight, expert_weight, w_gate, w_up, w_down, norm_gain, norm_bias
):
    tok_count = tokens.shape[0]
    expert_count = lax.axis_size("ep")
    capacity = min(tok_count // GROUPS, 3 * TOP_K * tok_count // (2 * expert_count))
    pair_count = tok_count * TOP_K
    flat_ids = expert_ids.reshape(pair_count)
    one_hot = (flat_ids[:, None] == jnp.arange(expert_count, dtype=jnp.int32)[None, :]).astype(
        jnp.float32
    )
    earlier = (jnp.arange(pair_count)[:, None] > jnp.arange(pair_count)[None, :]).astype(
        jnp.float32
    )
    prior_counts = jnp.dot(
        earlier, one_hot, preferred_element_type=jnp.float32, precision=lax.Precision.HIGHEST
    )
    slot_index = jnp.sum(prior_counts * one_hot, axis=1).astype(jnp.int32)
    position = flat_ids * capacity + slot_index
    owner_token = jnp.arange(pair_count, dtype=jnp.int32) // TOP_K
    slot_table = (
        jnp.full((expert_count * capacity,), tok_count, jnp.int32).at[position].set(owner_token)
    )
    gate_local = w_gate[0]
    up_local = w_up[0]
    down_local = w_down[0]
    padded = jnp.concatenate([tokens, jnp.zeros((1, tokens.shape[1]), tokens.dtype)], axis=0)
    outgoing = padded[slot_table].reshape(expert_count, capacity, tokens.shape[1])
    arrived = lax.all_to_all(outgoing, "ep", split_axis=0, concat_axis=0, tiled=True)
    sources, slot_count, slice_width = arrived.shape
    row_block = arrived.reshape(sources * slot_count, slice_width)
    row_piece = lax.all_gather(row_block, "tp", axis=1, tiled=True)
    gate_sum = jnp.dot(row_piece, gate_local, preferred_element_type=jnp.float32)
    up_sum = jnp.dot(row_piece, up_local, preferred_element_type=jnp.float32)
    hidden = (jax.nn.silu(gate_sum) * up_sum).astype(jnp.bfloat16)
    result = jnp.dot(
        lax.all_gather(hidden, "tp", axis=1, tiled=True),
        down_local,
        preferred_element_type=jnp.float32,
    )
    result = result.astype(jnp.bfloat16).reshape(sources, slot_count, down_local.shape[1])
    returned = lax.all_to_all(result, "ep", split_axis=0, concat_axis=0, tiled=True)
    flat_rows = returned.reshape(expert_count * capacity, returned.shape[2])
    picked = flat_rows[position].reshape(tok_count, TOP_K, returned.shape[2]).astype(jnp.float32)
    share_weight = (
        group_weight[:, None] * expert_weight / jnp.sum(expert_weight, axis=1, keepdims=True)
    )
    routed = jnp.einsum("tk,tkd->td", share_weight, picked)
    mixed = residual_scale * tokens.astype(jnp.float32) + routed
    first_sum, second_sum = lax.psum((jnp.sum(mixed, axis=1), jnp.sum(mixed * mixed, axis=1)), "tp")
    center = first_sum / D
    spread = second_sum / D - center * center
    centered = mixed - center[:, None]
    normed = (
        centered * lax.rsqrt(spread + norm_eps)[:, None] * norm_gain[None, :] + norm_bias[None, :]
    )
    return normed.astype(jnp.bfloat16)


MESH = pl.DeviceIdType.MESH
F32 = jnp.float32
BF16 = jnp.bfloat16
(TO_PLANE, SHARES, CORE_OWN, ACROSS_X, ACROSS_Y, CORE_X, CORE_Y, RELAY_X, RELAY_Y,
 CORE_RX, CORE_RY, HIDDEN_0, HIDDEN_1, RESULT, BACK, STATS, ACROSS_X2, ACROSS_Y2, RESULT_2,
 BACK_2) = range(20)
KINDS = 20


def flip(value, bits):
    bit = 1
    while bit <= bits:
        if bits & bit:
            value = value + bit - 2 * bit * lax.rem(lax.div(value, bit), 2)
        bit *= 2
    return value


def layer_kernel(
    n_plane, n_tp,
    tokens_hbm, ids_hbm, group_hbm, expert_hbm, gate_hbm, up_hbm, down_hbm,
    mixed_out, columns_out,
    tokens_ref, ids_ref, group_ref, expert_ref, mixed_ref,
    w_in, w_out, outgoing, share_out, share_in, rows, hidden, own_part, result_out, result_in,
    back_out, back_in, stats, send_sem, recv_sem, load_sem,
):
    ep = lax.axis_index("ep")
    q = lax.axis_index("tp")
    z, x = lax.div(ep, 2), lax.rem(ep, 2)
    ox = 1 - x
    q_core, q_y, q_diag = flip(q, 1), flip(q, 2), flip(q, 3)
    core_peer, y_peer, diag_peer = (ep, q_core), (ep, q_y), (ep, q_diag)
    x_peer = (z * 2 + ox, q)

    def plane_peer(d):
        return (flip(z, d) * 2 + x, q)

    tok, width = tokens_ref.shape
    cap = tok // n_plane
    half = cap // 2
    inner = gate_hbm.shape[2]

    inputs = [
        pltpu.make_async_copy(source, target, load_sem.at[3 + i])
        for i, (source, target) in enumerate((
            (ids_hbm, ids_ref), (tokens_hbm, tokens_ref), (group_hbm, group_ref),
            (expert_hbm, expert_ref),
        ))
    ]
    for load in inputs:
        load.start()

    barrier = pltpu.get_barrier_semaphore()
    partners = [plane_peer(d) for d in range(1, n_plane)] + [x_peer, core_peer, y_peer, diag_peer]
    for peer in partners:
        pl.semaphore_signal(barrier, inc=1, device_id=peer, device_id_type=MESH)

    loads = [
        pltpu.make_async_copy(gate_hbm.at[0], w_in.at[:, pl.ds(0, inner)], load_sem.at[0]),
        pltpu.make_async_copy(up_hbm.at[0], w_in.at[:, pl.ds(inner, inner)], load_sem.at[1]),
        pltpu.make_async_copy(down_hbm.at[0], w_out, load_sem.at[2]),
    ]
    for load in loads:
        load.start()

    inputs[0].wait()
    first = ids_ref[0:1, :]
    group_row = (first >> 1).astype(F32)
    on_lanes = jnp.broadcast_to(group_row, (tok, tok))
    on_rows = jnp.transpose(on_lanes)
    ii = lax.broadcasted_iota(jnp.int32, (tok, tok), 0)
    jj = lax.broadcasted_iota(jnp.int32, (tok, tok), 1)
    same = on_lanes == on_rows
    zero, one = jnp.zeros((tok, tok), F32), jnp.ones((tok, tok), F32)
    rank_row = jnp.sum(jnp.where(same & (ii < jj), one, zero), axis=0, keepdims=True)
    rank_col = jnp.sum(jnp.where(same & (jj < ii), one, zero), axis=1, keepdims=True)
    place_row = group_row * cap + rank_row
    place_col = on_rows[:, 0:1] * cap + rank_col
    to_slot = jnp.broadcast_to(place_row, (tok, tok)) == ii.astype(F32)
    to_token = jnp.broadcast_to(place_col, (tok, tok)) == jj.astype(F32)

    inputs[1].wait()
    sorted_rows = jnp.dot(
        jnp.where(to_slot, one, zero).astype(BF16), tokens_ref[...], preferred_element_type=F32
    ).astype(BF16)
    outgoing[...] = sorted_rows.reshape(n_plane, cap, width)
    rows[q, x, z] = outgoing[z]

    inputs[2].wait()
    inputs[3].wait()
    weights = expert_ref[...]
    share = group_ref[...] * weights / jnp.sum(weights, axis=0, keepdims=True)
    even = (first & 1) == 0
    share_a = jnp.where(even, share[0:1, :], share[1:2, :])
    share_b = jnp.where(even, share[1:2, :], share[0:1, :])
    slot_a = jnp.sum(jnp.where(to_slot, jnp.broadcast_to(share_a, (tok, tok)), zero), axis=1, keepdims=True)
    slot_b = jnp.sum(jnp.where(to_slot, jnp.broadcast_to(share_b, (tok, tok)), zero), axis=1, keepdims=True)
    lane = lax.broadcasted_iota(jnp.int32, (tok, 128), 1)
    share_out[...] = jnp.where(lane < 64, slot_a, slot_b).reshape(n_plane, cap, 128)
    share_in[z] = share_out[z]

    pl.semaphore_wait(barrier, len(partners))

    started = []

    def copy(src, dst, kind, j, peer):
        return pltpu.make_async_remote_copy(
            src_ref=src, dst_ref=dst, send_sem=send_sem.at[kind, j], recv_sem=recv_sem.at[kind, j],
            device_id=peer, device_id_type=MESH,
        )

    def send(src, dst, kind, j, peer):
        c = copy(src, dst, kind, j, peer)
        c.start()
        started.append(c)

    def arrived(dst, kind, j):
        copy(dst, dst, kind, j, core_peer).wait_recv()

    for d in range(1, n_plane):
        send(outgoing.at[flip(z, d)], rows.at[q, x, z], TO_PLANE, d, plane_peer(d))

    low, high = pl.ds(0, half), pl.ds(half, half)

    def spread_own(j):
        block = rows.at[q, x, flip(z, j)]
        if j:
            arrived(block, TO_PLANE, j)
        send(block.at[low], block.at[low], ACROSS_X, j, x_peer)
        send(block.at[high], block.at[high], ACROSS_Y, j, y_peer)
        send(block.at[high], block.at[high], ACROSS_X2, j, x_peer)
        send(block.at[low], block.at[low], ACROSS_Y2, j, y_peer)
        send(block, block, CORE_OWN, j, core_peer)

    def pass_on(j):
        zz = flip(z, j)
        over_x, over_y = rows.at[q, ox, zz], rows.at[q_y, x, zz]
        arrived(over_x.at[low], ACROSS_X, j)
        send(over_x.at[low], over_x.at[low], RELAY_Y, j, y_peer)
        arrived(over_y.at[high], ACROSS_Y, j)
        send(over_y.at[high], over_y.at[high], RELAY_X, j, x_peer)
        arrived(over_x.at[high], ACROSS_X2, j)
        send(over_x, over_x, CORE_X, j, core_peer)
        arrived(over_y.at[low], ACROSS_Y2, j)
        send(over_y, over_y, CORE_Y, j, core_peer)

    def pass_relayed(j):
        block = rows.at[q_y, ox, flip(z, j)]
        arrived(block.at[low], RELAY_Y, j)
        send(block.at[low], block.at[low], CORE_RY, j, core_peer)
        arrived(block.at[high], RELAY_X, j)
        send(block.at[high], block.at[high], CORE_RX, j, core_peer)

    for step in range(n_plane + 1):
        if step < n_plane:
            spread_own(step)
        if step >= 1:
            pass_on(step - 1)
        if step >= 2:
            pass_relayed(step - 2)

    for d in range(1, n_plane):
        send(share_out.at[flip(z, d)], share_in.at[z], SHARES, d, plane_peer(d))

    def sums_of(column, quarter):
        part = rows[quarter, column].reshape(tok, width)
        w = w_in[pl.ds(pl.multiple_of(quarter * width, width), width), :]
        return jnp.dot(part, w, preferred_element_type=F32)

    def finish_hidden(total, column, kind):
        gate, up = total[:, :inner], total[:, inner:]
        hidden[column, q] = (gate / (1.0 + jnp.exp(-gate)) * up).astype(BF16)
        block = hidden.at[column, q]
        for d, peer in ((2, y_peer), (3, diag_peer), (1, core_peer)):
            send(block, block, kind, d, peer)

    def project(column, kind):
        for d in range(1, n_tp):
            arrived(hidden.at[column, flip(q, d)], kind, d)
        h = jnp.concatenate([hidden[column, t] for t in range(n_tp)], axis=1)
        return jnp.dot(h, w_out[...], preferred_element_type=F32).astype(BF16)

    loads[0].wait()
    loads[1].wait()
    total = sums_of(x, q) + sums_of(x, q_y)
    other = sums_of(ox, q)
    for j in range(n_plane):
        arrived(rows.at[q_core, x, flip(z, j)], CORE_OWN, j)
        arrived(rows.at[q_diag, x, flip(z, j)], CORE_Y, j)
    total = total + sums_of(x, q_core) + sums_of(x, q_diag)
    finish_hidden(total, x, HIDDEN_0)
    pass_relayed(n_plane - 1)
    for j in range(n_plane):
        arrived(rows.at[q_core, ox, flip(z, j)], CORE_X, j)
    other = other + sums_of(ox, q_core) + sums_of(ox, q_y)
    for j in range(n_plane):
        block = rows.at[q_diag, ox, flip(z, j)]
        arrived(block.at[low], CORE_RY, j)
        arrived(block.at[high], CORE_RX, j)
    other = other + sums_of(ox, q_diag)
    finish_hidden(other, ox, HIDDEN_1)

    loads[2].wait()
    for d in range(1, n_plane):
        arrived(share_in.at[flip(z, d)], SHARES, d)
    shares = share_in[...].reshape(tok, 128)
    is_first = x == 0
    share_own = jnp.where(is_first, shares[:, 0:1], shares[:, 64:65])
    share_other = jnp.where(is_first, shares[:, 64:65], shares[:, 0:1])
    own_part[...] = (project(x, HIDDEN_0).astype(F32) * share_own).reshape(n_plane, cap, width)
    share_in[...] = jnp.broadcast_to(share_other, (tok, 128)).reshape(n_plane, cap, 128)

    result_out[...] = project(ox, HIDDEN_1).reshape(n_plane, cap, width)
    order = tuple(range(n_plane - 1, -1, -1))
    pieces = ((low, 0, RESULT, BACK), (high, half, RESULT_2, BACK_2))
    for j in order:
        zz = flip(z, j)
        for part, _, there, _ in pieces:
            send(result_out.at[zz, part], result_in.at[zz, part], there, j, x_peer)
    for j in order:
        zz = flip(z, j)
        for part, at, there, home in pieces:
            arrived(result_in.at[zz, part], there, j)
            scaled = result_in[zz, at:at + half].astype(F32) * share_in[zz, at:at + half][:, 0:1]
            mixed_rows = (own_part[zz, at:at + half] + scaled).astype(BF16)
            if j:
                back_out[zz, at:at + half] = mixed_rows
                send(back_out.at[zz, part], back_in.at[z, part], home, j, plane_peer(j))
            else:
                back_in[z, at:at + half] = mixed_rows
    for j in order:
        if j:
            for part, _, _, home in pieces:
                arrived(back_in.at[flip(z, j), part], home, j)
    routed = jnp.dot(
        jnp.where(to_token, one, zero).astype(BF16),
        back_in[...].reshape(tok, width),
        preferred_element_type=F32,
    )
    mixed = residual_scale * tokens_ref[...].astype(F32) + routed
    mixed_ref[...] = mixed
    keep = pltpu.make_async_copy(mixed_ref, mixed_out, load_sem.at[7])
    keep.start()
    total_col = jnp.sum(mixed, axis=1, keepdims=True)
    centered = mixed - total_col / width
    square_col = jnp.sum(centered * centered, axis=1, keepdims=True)
    lane = lax.broadcasted_iota(jnp.int32, (tok, 128), 1)
    stats[q] = jnp.transpose(jnp.where(lane == 0, total_col, square_col))[0:8, :]
    for d, peer in ((3, diag_peer), (2, y_peer), (1, core_peer)):
        send(stats.at[q], stats.at[q], STATS, d, peer)
    for d in range(1, n_tp):
        arrived(stats.at[flip(q, d)], STATS, d)
    pieces = [stats[t] for t in range(n_tp)]
    full = width * n_tp
    center = sum(p[0:1, :] for p in pieces) / full
    spread = sum(p[1:2, :] + width * jnp.square(p[0:1, :] / width - center) for p in pieces) / full
    scale = lax.rsqrt(spread + norm_eps)
    sub = lax.broadcasted_iota(jnp.int32, (128, tok), 0)
    columns_out[...] = jnp.transpose(jnp.where(sub == 0, center, scale))
    keep.wait()
    for c in started:
        c.wait_send()


def norm_kernel(mixed_ref, columns_ref, gain_ref, bias_ref, out_ref):
    center, scale = columns_ref[:, 0:1], columns_ref[:, 1:2]
    out_ref[...] = (
        (mixed_ref[...] - center) * scale * gain_ref[...] + bias_ref[...]
    ).astype(BF16)


def pair_groups(
    tokens, expert_ids, group_weight, expert_weight, w_gate, w_up, w_down, norm_gain, norm_bias
):
    tok, width = tokens.shape
    n_plane = lax.axis_size("ep") // TOP_K
    n_tp = lax.axis_size("tp")
    cap = tok // n_plane
    inner = w_gate.shape[2]
    vmem = pl.BlockSpec(memory_space=pltpu.VMEM)
    hbm = pl.BlockSpec(memory_space=pltpu.HBM)
    mixed, columns = pl.pallas_call(
        functools.partial(layer_kernel, n_plane, n_tp),
        out_shape=(
            jax.ShapeDtypeStruct((tok, width), F32), jax.ShapeDtypeStruct((tok, 128), F32)
        ),
        in_specs=[hbm] * 7,
        out_specs=(pl.BlockSpec(memory_space=pl.ANY), vmem),
        scratch_shapes=[
            pltpu.VMEM((tok, width), BF16),
            pltpu.VMEM((TOP_K, tok), jnp.int32),
            pltpu.VMEM((1, tok), F32),
            pltpu.VMEM((TOP_K, tok), F32),
            pltpu.VMEM((tok, width), F32),
            pltpu.VMEM((w_gate.shape[1], 2 * inner), BF16),
            pltpu.VMEM(w_down.shape[1:], BF16),
            pltpu.VMEM((n_plane, cap, width), BF16),
            pltpu.VMEM((n_plane, cap, 128), F32),
            pltpu.VMEM((n_plane, cap, 128), F32),
            pltpu.VMEM((n_tp, 2, n_plane, cap, width), BF16),
            pltpu.VMEM((2, n_tp, tok, inner), BF16),
            pltpu.VMEM((n_plane, cap, width), F32),
            pltpu.VMEM((n_plane, cap, width), BF16),
            pltpu.VMEM((n_plane, cap, width), BF16),
            pltpu.VMEM((n_plane, cap, width), BF16),
            pltpu.VMEM((n_plane, cap, width), BF16),
            pltpu.VMEM((n_tp, 8, tok), F32),
            pltpu.SemaphoreType.DMA((KINDS, 4)),
            pltpu.SemaphoreType.DMA((KINDS, 4)),
            pltpu.SemaphoreType.DMA((8,)),
        ],
        compiler_params=pltpu.CompilerParams(
            collective_id=0, has_side_effects=True, vmem_limit_bytes=56 * 2**20
        ),
        name="layer",
    )(
        tokens, expert_ids.T, group_weight[None, :], expert_weight.T, w_gate, w_up, w_down
    )
    return pl.pallas_call(
        norm_kernel,
        out_shape=jax.ShapeDtypeStruct((tok, width), BF16),
        in_specs=[vmem] * 4,
        out_specs=vmem,
        compiler_params=pltpu.CompilerParams(vmem_limit_bytes=56 * 2**20),
        name="norm",
    )(mixed, columns, norm_gain[None, :], norm_bias[None, :])


def solution(mesh):
    n_ep, n_tp = mesh.shape["ep"], mesh.shape["tp"]
    pairs = TOP_K == 2 and n_ep == GROUPS * TOP_K and n_tp == 4
    return jax.shard_map(
        pair_groups if pairs else on_device,
        mesh=mesh,
        in_specs=(
            P("ep", "tp"),
            P("ep", None),
            P("ep"),
            P("ep", None),
            P("ep", None, "tp"),
            P("ep", None, "tp"),
            P("ep", None, "tp"),
            P("tp"),
            P("tp"),
        ),
        out_specs=P("ep", "tp"),
        check_vma=False,
    )
```

```python
import functools

import jax
import jax.numpy as jnp
from jax import lax
from jax.experimental import pallas as pl
from jax.experimental.pallas import tpu as pltpu
from jax.sharding import PartitionSpec as P

D = 4096
GROUPS = 4
TOP_K = 2


residual_scale = 2.0**0.5
norm_eps = 1e-05


def on_device(
    tokens, expert_ids, group_weight, expert_weight, w_gate, w_up, w_down, norm_gain, norm_bias
):
    tok_count = tokens.shape[0]
    expert_count = lax.axis_size("ep")
    capacity = min(tok_count // GROUPS, 3 * TOP_K * tok_count // (2 * expert_count))
    pair_count = tok_count * TOP_K
    flat_ids = expert_ids.reshape(pair_count)
    one_hot = (flat_ids[:, None] == jnp.arange(expert_count, dtype=jnp.int32)[None, :]).astype(
        jnp.float32
    )
    earlier = (jnp.arange(pair_count)[:, None] > jnp.arange(pair_count)[None, :]).astype(
        jnp.float32
    )
    prior_counts = jnp.dot(
        earlier, one_hot, preferred_element_type=jnp.float32, precision=lax.Precision.HIGHEST
    )
    slot_index = jnp.sum(prior_counts * one_hot, axis=1).astype(jnp.int32)
    position = flat_ids * capacity + slot_index
    owner_token = jnp.arange(pair_count, dtype=jnp.int32) // TOP_K
    slot_table = (
        jnp.full((expert_count * capacity,), tok_count, jnp.int32).at[position].set(owner_token)
    )
    gate_local = w_gate[0]
    up_local = w_up[0]
    down_local = w_down[0]
    padded = jnp.concatenate([tokens, jnp.zeros((1, tokens.shape[1]), tokens.dtype)], axis=0)
    outgoing = padded[slot_table].reshape(expert_count, capacity, tokens.shape[1])
    arrived = lax.all_to_all(outgoing, "ep", split_axis=0, concat_axis=0, tiled=True)
    sources, slot_count, slice_width = arrived.shape
    row_block = arrived.reshape(sources * slot_count, slice_width)
    row_piece = lax.all_gather(row_block, "tp", axis=1, tiled=True)
    gate_sum = jnp.dot(row_piece, gate_local, preferred_element_type=jnp.float32)
    up_sum = jnp.dot(row_piece, up_local, preferred_element_type=jnp.float32)
    hidden = (jax.nn.silu(gate_sum) * up_sum).astype(jnp.bfloat16)
    result = jnp.dot(
        lax.all_gather(hidden, "tp", axis=1, tiled=True),
        down_local,
        preferred_element_type=jnp.float32,
    )
    result = result.astype(jnp.bfloat16).reshape(sources, slot_count, down_local.shape[1])
    returned = lax.all_to_all(result, "ep", split_axis=0, concat_axis=0, tiled=True)
    flat_rows = returned.reshape(expert_count * capacity, returned.shape[2])
    picked = flat_rows[position].reshape(tok_count, TOP_K, returned.shape[2]).astype(jnp.float32)
    share_weight = (
        group_weight[:, None] * expert_weight / jnp.sum(expert_weight, axis=1, keepdims=True)
    )
    routed = jnp.einsum("tk,tkd->td", share_weight, picked)
    mixed = residual_scale * tokens.astype(jnp.float32) + routed
    first_sum, second_sum = lax.psum((jnp.sum(mixed, axis=1), jnp.sum(mixed * mixed, axis=1)), "tp")
    center = first_sum / D
    spread = second_sum / D - center * center
    centered = mixed - center[:, None]
    normed = (
        centered * lax.rsqrt(spread + norm_eps)[:, None] * norm_gain[None, :] + norm_bias[None, :]
    )
    return normed.astype(jnp.bfloat16)


MESH = pl.DeviceIdType.MESH
F32 = jnp.float32
BF16 = jnp.bfloat16
(TO_PLANE, SHARES, CORE_OWN, ACROSS_X, ACROSS_Y, CORE_X, CORE_Y, RELAY_X, RELAY_Y,
 CORE_RX, CORE_RY, HIDDEN_0, HIDDEN_1, RESULT, BACK, STATS, ACROSS_X2, ACROSS_Y2, RESULT_2,
 BACK_2, TO_PLANE_2) = range(21)
KINDS = 21


def flip(value, bits):
    bit = 1
    while bit <= bits:
        if bits & bit:
            value = value + bit - 2 * bit * lax.rem(lax.div(value, bit), 2)
        bit *= 2
    return value


def layer_kernel(
    n_plane, n_tp,
    tokens_hbm, ids_hbm, group_hbm, expert_hbm, gate_hbm, up_hbm, down_hbm,
    mixed_out, columns_out,
    tokens_ref, ids_ref, group_ref, expert_ref, mixed_ref,
    w_in, w_out, outgoing, share_out, share_in, rows, hidden, own_part, result_out, result_in,
    back_out, back_in, stats, send_sem, recv_sem, load_sem,
):
    ep = lax.axis_index("ep")
    q = lax.axis_index("tp")
    z, x = lax.div(ep, 2), lax.rem(ep, 2)
    ox = 1 - x
    q_core, q_y, q_diag = flip(q, 1), flip(q, 2), flip(q, 3)
    core_peer, y_peer, diag_peer = (ep, q_core), (ep, q_y), (ep, q_diag)
    x_peer = (z * 2 + ox, q)

    def plane_peer(d):
        return (flip(z, d) * 2 + x, q)

    tok, width = tokens_ref.shape
    cap = tok // n_plane
    half = cap // 2
    inner = gate_hbm.shape[2]

    inputs = [
        pltpu.make_async_copy(source, target, load_sem.at[3 + i])
        for i, (source, target) in enumerate((
            (ids_hbm, ids_ref), (tokens_hbm, tokens_ref), (group_hbm, group_ref),
            (expert_hbm, expert_ref),
        ))
    ]
    for load in inputs:
        load.start()

    barrier = pltpu.get_barrier_semaphore()
    partners = [plane_peer(d) for d in range(1, n_plane)] + [x_peer, core_peer, y_peer, diag_peer]
    for peer in partners:
        pl.semaphore_signal(barrier, inc=1, device_id=peer, device_id_type=MESH)

    loads = [
        pltpu.make_async_copy(gate_hbm.at[0], w_in.at[:, pl.ds(0, inner)], load_sem.at[0]),
        pltpu.make_async_copy(up_hbm.at[0], w_in.at[:, pl.ds(inner, inner)], load_sem.at[1]),
        pltpu.make_async_copy(down_hbm.at[0], w_out, load_sem.at[2]),
    ]
    for load in loads:
        load.start()

    inputs[0].wait()
    first = ids_ref[0:1, :]
    group_row = (first >> 1).astype(F32)
    on_lanes = jnp.broadcast_to(group_row, (tok, tok))
    on_rows = jnp.transpose(on_lanes)
    ii = lax.broadcasted_iota(jnp.int32, (tok, tok), 0)
    jj = lax.broadcasted_iota(jnp.int32, (tok, tok), 1)
    same = on_lanes == on_rows
    zero, one = jnp.zeros((tok, tok), F32), jnp.ones((tok, tok), F32)
    rank_row = jnp.sum(jnp.where(same & (ii < jj), one, zero), axis=0, keepdims=True)
    rank_col = jnp.sum(jnp.where(same & (jj < ii), one, zero), axis=1, keepdims=True)
    place_row = group_row * cap + rank_row
    place_col = on_rows[:, 0:1] * cap + rank_col
    to_slot = jnp.broadcast_to(place_row, (tok, tok)) == ii.astype(F32)
    to_token = jnp.broadcast_to(place_col, (tok, tok)) == jj.astype(F32)

    inputs[1].wait()
    sorted_rows = jnp.dot(
        jnp.where(to_slot, one, zero).astype(BF16), tokens_ref[...], preferred_element_type=F32
    ).astype(BF16)
    outgoing[...] = sorted_rows.reshape(n_plane, cap, width)
    rows[q, x, z] = outgoing[z]

    inputs[2].wait()
    inputs[3].wait()
    weights = expert_ref[...]
    share = group_ref[...] * weights / jnp.sum(weights, axis=0, keepdims=True)
    even = (first & 1) == 0
    share_a = jnp.where(even, share[0:1, :], share[1:2, :])
    share_b = jnp.where(even, share[1:2, :], share[0:1, :])
    slot_a = jnp.sum(jnp.where(to_slot, jnp.broadcast_to(share_a, (tok, tok)), zero), axis=1, keepdims=True)
    slot_b = jnp.sum(jnp.where(to_slot, jnp.broadcast_to(share_b, (tok, tok)), zero), axis=1, keepdims=True)
    lane = lax.broadcasted_iota(jnp.int32, (tok, 128), 1)
    share_out[...] = jnp.where(lane < 64, slot_a, slot_b).reshape(n_plane, cap, 128)
    share_in[z] = share_out[z]

    pl.semaphore_wait(barrier, len(partners))

    started = []

    def copy(src, dst, kind, j, peer):
        return pltpu.make_async_remote_copy(
            src_ref=src, dst_ref=dst, send_sem=send_sem.at[kind, j], recv_sem=recv_sem.at[kind, j],
            device_id=peer, device_id_type=MESH,
        )

    def send(src, dst, kind, j, peer):
        c = copy(src, dst, kind, j, peer)
        c.start()
        started.append(c)

    def arrived(dst, kind, j):
        copy(dst, dst, kind, j, core_peer).wait_recv()

    low, high = pl.ds(0, half), pl.ds(half, half)
    for d in range(1, n_plane):
        for part, kind in ((low, TO_PLANE), (high, TO_PLANE_2)):
            send(outgoing.at[flip(z, d), part], rows.at[q, x, z, part], kind, d, plane_peer(d))

    def spread_own(j):
        block = rows.at[q, x, flip(z, j)]
        if j:
            arrived(block.at[low], TO_PLANE, j)
        send(block.at[low], block.at[low], ACROSS_X, j, x_peer)
        if j:
            send(block.at[low], block.at[low], ACROSS_Y2, j, y_peer)
            arrived(block.at[high], TO_PLANE_2, j)
        send(block.at[high], block.at[high], ACROSS_Y, j, y_peer)
        send(block.at[high], block.at[high], ACROSS_X2, j, x_peer)
        if not j:
            send(block.at[low], block.at[low], ACROSS_Y2, j, y_peer)
        send(block, block, CORE_OWN, j, core_peer)

    def pass_on(j):
        zz = flip(z, j)
        over_x, over_y = rows.at[q, ox, zz], rows.at[q_y, x, zz]
        arrived(over_x.at[low], ACROSS_X, j)
        send(over_x.at[low], over_x.at[low], RELAY_Y, j, y_peer)
        arrived(over_y.at[high], ACROSS_Y, j)
        send(over_y.at[high], over_y.at[high], RELAY_X, j, x_peer)
        arrived(over_x.at[high], ACROSS_X2, j)
        send(over_x, over_x, CORE_X, j, core_peer)
        arrived(over_y.at[low], ACROSS_Y2, j)
        send(over_y, over_y, CORE_Y, j, core_peer)

    def pass_relayed(j):
        block = rows.at[q_y, ox, flip(z, j)]
        arrived(block.at[low], RELAY_Y, j)
        send(block.at[low], block.at[low], CORE_RY, j, core_peer)
        arrived(block.at[high], RELAY_X, j)
        send(block.at[high], block.at[high], CORE_RX, j, core_peer)

    for step in range(n_plane + 1):
        if step < n_plane:
            spread_own(step)
        if step >= 1:
            pass_on(step - 1)
        if step >= 2:
            pass_relayed(step - 2)

    for d in range(1, n_plane):
        send(share_out.at[flip(z, d)], share_in.at[z], SHARES, d, plane_peer(d))

    def sums_of(column, quarter):
        part = rows[quarter, column].reshape(tok, width)
        w = w_in[pl.ds(pl.multiple_of(quarter * width, width), width), :]
        return jnp.dot(part, w, preferred_element_type=F32)

    def finish_hidden(total, column, kind):
        gate, up = total[:, :inner], total[:, inner:]
        hidden[column, q] = (gate / (1.0 + jnp.exp(-gate)) * up).astype(BF16)
        block = hidden.at[column, q]
        for d, peer in ((2, y_peer), (3, diag_peer), (1, core_peer)):
            send(block, block, kind, d, peer)

    def project(column, kind):
        for d in range(1, n_tp):
            arrived(hidden.at[column, flip(q, d)], kind, d)
        h = jnp.concatenate([hidden[column, t] for t in range(n_tp)], axis=1)
        return jnp.dot(h, w_out[...], preferred_element_type=F32).astype(BF16)

    loads[0].wait()
    loads[1].wait()
    total = sums_of(x, q) + sums_of(x, q_y)
    other = sums_of(ox, q)
    for j in range(n_plane):
        arrived(rows.at[q_core, x, flip(z, j)], CORE_OWN, j)
        arrived(rows.at[q_diag, x, flip(z, j)], CORE_Y, j)
    total = total + sums_of(x, q_core) + sums_of(x, q_diag)
    finish_hidden(total, x, HIDDEN_0)
    pass_relayed(n_plane - 1)
    for j in range(n_plane):
        arrived(rows.at[q_core, ox, flip(z, j)], CORE_X, j)
    other = other + sums_of(ox, q_core) + sums_of(ox, q_y)
    for j in range(n_plane):
        block = rows.at[q_diag, ox, flip(z, j)]
        arrived(block.at[low], CORE_RY, j)
        arrived(block.at[high], CORE_RX, j)
    other = other + sums_of(ox, q_diag)
    finish_hidden(other, ox, HIDDEN_1)

    loads[2].wait()
    for d in range(1, n_plane):
        arrived(share_in.at[flip(z, d)], SHARES, d)
    shares = share_in[...].reshape(tok, 128)
    is_first = x == 0
    share_own = jnp.where(is_first, shares[:, 0:1], shares[:, 64:65])
    share_other = jnp.where(is_first, shares[:, 64:65], shares[:, 0:1])
    own_part[...] = (project(x, HIDDEN_0).astype(F32) * share_own).reshape(n_plane, cap, width)
    share_in[...] = jnp.broadcast_to(share_other, (tok, 128)).reshape(n_plane, cap, 128)

    result_out[...] = project(ox, HIDDEN_1).reshape(n_plane, cap, width)
    order = tuple(range(n_plane - 1, -1, -1))
    pieces = ((low, 0, RESULT, BACK), (high, half, RESULT_2, BACK_2))
    for j in order:
        zz = flip(z, j)
        for part, _, there, _ in pieces:
            send(result_out.at[zz, part], result_in.at[zz, part], there, j, x_peer)
    for j in order:
        zz = flip(z, j)
        for part, at, there, home in pieces:
            arrived(result_in.at[zz, part], there, j)
            scaled = result_in[zz, at:at + half].astype(F32) * share_in[zz, at:at + half][:, 0:1]
            mixed_rows = (own_part[zz, at:at + half] + scaled).astype(BF16)
            if j:
                back_out[zz, at:at + half] = mixed_rows
                send(back_out.at[zz, part], back_in.at[z, part], home, j, plane_peer(j))
            else:
                back_in[z, at:at + half] = mixed_rows
    for j in order:
        if j:
            for part, _, _, home in pieces:
                arrived(back_in.at[flip(z, j), part], home, j)
    routed = jnp.dot(
        jnp.where(to_token, one, zero).astype(BF16),
        back_in[...].reshape(tok, width),
        preferred_element_type=F32,
    )
    mixed = residual_scale * tokens_ref[...].astype(F32) + routed
    mixed_ref[...] = mixed
    keep = pltpu.make_async_copy(mixed_ref, mixed_out, load_sem.at[7])
    keep.start()
    total_col = jnp.sum(mixed, axis=1, keepdims=True)
    centered = mixed - total_col / width
    square_col = jnp.sum(centered * centered, axis=1, keepdims=True)
    lane = lax.broadcasted_iota(jnp.int32, (tok, 128), 1)
    stats[q] = jnp.transpose(jnp.where(lane == 0, total_col, square_col))[0:8, :]
    for d, peer in ((3, diag_peer), (2, y_peer), (1, core_peer)):
        send(stats.at[q], stats.at[q], STATS, d, peer)
    for d in range(1, n_tp):
        arrived(stats.at[flip(q, d)], STATS, d)
    pieces = [stats[t] for t in range(n_tp)]
    full = width * n_tp
    center = sum(p[0:1, :] for p in pieces) / full
    spread = sum(p[1:2, :] + width * jnp.square(p[0:1, :] / width - center) for p in pieces) / full
    scale = lax.rsqrt(spread + norm_eps)
    sub = lax.broadcasted_iota(jnp.int32, (128, tok), 0)
    columns_out[...] = jnp.transpose(jnp.where(sub == 0, center, scale))
    keep.wait()
    for c in started:
        c.wait_send()


def norm_kernel(mixed_ref, columns_ref, gain_ref, bias_ref, out_ref):
    center, scale = columns_ref[:, 0:1], columns_ref[:, 1:2]
    out_ref[...] = (
        (mixed_ref[...] - center) * scale * gain_ref[...] + bias_ref[...]
    ).astype(BF16)


def pair_groups(
    tokens, expert_ids, group_weight, expert_weight, w_gate, w_up, w_down, norm_gain, norm_bias
):
    tok, width = tokens.shape
    n_plane = lax.axis_size("ep") // TOP_K
    n_tp = lax.axis_size("tp")
    cap = tok // n_plane
    inner = w_gate.shape[2]
    vmem = pl.BlockSpec(memory_space=pltpu.VMEM)
    hbm = pl.BlockSpec(memory_space=pltpu.HBM)
    mixed, columns = pl.pallas_call(
        functools.partial(layer_kernel, n_plane, n_tp),
        out_shape=(
            jax.ShapeDtypeStruct((tok, width), F32), jax.ShapeDtypeStruct((tok, 128), F32)
        ),
        in_specs=[hbm] * 7,
        out_specs=(pl.BlockSpec(memory_space=pl.ANY), vmem),
        scratch_shapes=[
            pltpu.VMEM((tok, width), BF16),
            pltpu.VMEM((TOP_K, tok), jnp.int32),
            pltpu.VMEM((1, tok), F32),
            pltpu.VMEM((TOP_K, tok), F32),
            pltpu.VMEM((tok, width), F32),
            pltpu.VMEM((w_gate.shape[1], 2 * inner), BF16),
            pltpu.VMEM(w_down.shape[1:], BF16),
            pltpu.VMEM((n_plane, cap, width), BF16),
            pltpu.VMEM((n_plane, cap, 128), F32),
            pltpu.VMEM((n_plane, cap, 128), F32),
            pltpu.VMEM((n_tp, 2, n_plane, cap, width), BF16),
            pltpu.VMEM((2, n_tp, tok, inner), BF16),
            pltpu.VMEM((n_plane, cap, width), F32),
            pltpu.VMEM((n_plane, cap, width), BF16),
            pltpu.VMEM((n_plane, cap, width), BF16),
            pltpu.VMEM((n_plane, cap, width), BF16),
            pltpu.VMEM((n_plane, cap, width), BF16),
            pltpu.VMEM((n_tp, 8, tok), F32),
            pltpu.SemaphoreType.DMA((KINDS, 4)),
            pltpu.SemaphoreType.DMA((KINDS, 4)),
            pltpu.SemaphoreType.DMA((8,)),
        ],
        compiler_params=pltpu.CompilerParams(
            collective_id=0, has_side_effects=True, vmem_limit_bytes=53 * 2**20
        ),
        name="layer",
    )(
        tokens, expert_ids.T, group_weight[None, :], expert_weight.T, w_gate, w_up, w_down
    )
    return pl.pallas_call(
        norm_kernel,
        out_shape=jax.ShapeDtypeStruct((tok, width), BF16),
        in_specs=[vmem] * 4,
        out_specs=vmem,
        compiler_params=pltpu.CompilerParams(vmem_limit_bytes=8 * 2**20),
        name="norm",
    )(mixed, columns, norm_gain[None, :], norm_bias[None, :])


def solution(mesh):
    n_ep, n_tp = mesh.shape["ep"], mesh.shape["tp"]
    pairs = TOP_K == 2 and n_ep == GROUPS * TOP_K and n_tp == 4
    return jax.shard_map(
        pair_groups if pairs else on_device,
        mesh=mesh,
        in_specs=(
            P("ep", "tp"),
            P("ep", None),
            P("ep"),
            P("ep", None),
            P("ep", None, "tp"),
            P("ep", None, "tp"),
            P("ep", None, "tp"),
            P("tp"),
            P("tp"),
        ),
        out_specs=P("ep", "tp"),
        check_vma=False,
    )
```

```python
import functools

import jax
import jax.numpy as jnp
from jax import lax
from jax.experimental import pallas as pl
from jax.experimental.pallas import tpu as pltpu
from jax.sharding import PartitionSpec as P

D = 4096
GROUPS = 4
TOP_K = 2


residual_scale = 2.0**0.5
norm_eps = 1e-05


def on_device(
    tokens, expert_ids, group_weight, expert_weight, w_gate, w_up, w_down, norm_gain, norm_bias
):
    tok_count = tokens.shape[0]
    expert_count = lax.axis_size("ep")
    capacity = min(tok_count // GROUPS, 3 * TOP_K * tok_count // (2 * expert_count))
    pair_count = tok_count * TOP_K
    flat_ids = expert_ids.reshape(pair_count)
    one_hot = (flat_ids[:, None] == jnp.arange(expert_count, dtype=jnp.int32)[None, :]).astype(
        jnp.float32
    )
    earlier = (jnp.arange(pair_count)[:, None] > jnp.arange(pair_count)[None, :]).astype(
        jnp.float32
    )
    prior_counts = jnp.dot(
        earlier, one_hot, preferred_element_type=jnp.float32, precision=lax.Precision.HIGHEST
    )
    slot_index = jnp.sum(prior_counts * one_hot, axis=1).astype(jnp.int32)
    position = flat_ids * capacity + slot_index
    owner_token = jnp.arange(pair_count, dtype=jnp.int32) // TOP_K
    slot_table = (
        jnp.full((expert_count * capacity,), tok_count, jnp.int32).at[position].set(owner_token)
    )
    gate_local = w_gate[0]
    up_local = w_up[0]
    down_local = w_down[0]
    padded = jnp.concatenate([tokens, jnp.zeros((1, tokens.shape[1]), tokens.dtype)], axis=0)
    outgoing = padded[slot_table].reshape(expert_count, capacity, tokens.shape[1])
    arrived = lax.all_to_all(outgoing, "ep", split_axis=0, concat_axis=0, tiled=True)
    sources, slot_count, slice_width = arrived.shape
    row_block = arrived.reshape(sources * slot_count, slice_width)
    row_piece = lax.all_gather(row_block, "tp", axis=1, tiled=True)
    gate_sum = jnp.dot(row_piece, gate_local, preferred_element_type=jnp.float32)
    up_sum = jnp.dot(row_piece, up_local, preferred_element_type=jnp.float32)
    hidden = (jax.nn.silu(gate_sum) * up_sum).astype(jnp.bfloat16)
    result = jnp.dot(
        lax.all_gather(hidden, "tp", axis=1, tiled=True),
        down_local,
        preferred_element_type=jnp.float32,
    )
    result = result.astype(jnp.bfloat16).reshape(sources, slot_count, down_local.shape[1])
    returned = lax.all_to_all(result, "ep", split_axis=0, concat_axis=0, tiled=True)
    flat_rows = returned.reshape(expert_count * capacity, returned.shape[2])
    picked = flat_rows[position].reshape(tok_count, TOP_K, returned.shape[2]).astype(jnp.float32)
    share_weight = (
        group_weight[:, None] * expert_weight / jnp.sum(expert_weight, axis=1, keepdims=True)
    )
    routed = jnp.einsum("tk,tkd->td", share_weight, picked)
    mixed = residual_scale * tokens.astype(jnp.float32) + routed
    first_sum, second_sum = lax.psum((jnp.sum(mixed, axis=1), jnp.sum(mixed * mixed, axis=1)), "tp")
    center = first_sum / D
    spread = second_sum / D - center * center
    centered = mixed - center[:, None]
    normed = (
        centered * lax.rsqrt(spread + norm_eps)[:, None] * norm_gain[None, :] + norm_bias[None, :]
    )
    return normed.astype(jnp.bfloat16)


MESH = pl.DeviceIdType.MESH
F32 = jnp.float32
BF16 = jnp.bfloat16
(TO_PLANE, SHARES, CORE_OWN, ACROSS_X, ACROSS_Y, CORE_X, CORE_Y, RELAY_X, RELAY_Y,
 CORE_RX, CORE_RY, HIDDEN_0, HIDDEN_1, RESULT, BACK, STATS, ACROSS_X2, ACROSS_Y2, RESULT_2,
 BACK_2, TO_PLANE_2) = range(21)
KINDS = 21


def flip(value, bits):
    bit = 1
    while bit <= bits:
        if bits & bit:
            value = value + bit - 2 * bit * lax.rem(lax.div(value, bit), 2)
        bit *= 2
    return value


def layer_kernel(
    n_plane, n_tp,
    tokens_hbm, ids_hbm, group_hbm, expert_hbm, gate_hbm, up_hbm, down_hbm,
    mixed_out, columns_out,
    tokens_ref, ids_ref, group_ref, expert_ref, mixed_ref,
    w_in, w_out, outgoing, share_out, share_in, rows, hidden, own_part, result_out, result_in,
    back_out, back_in, stats, send_sem, recv_sem, load_sem,
):
    ep = lax.axis_index("ep")
    q = lax.axis_index("tp")
    z, x = lax.div(ep, 2), lax.rem(ep, 2)
    ox = 1 - x
    q_core, q_y, q_diag = flip(q, 1), flip(q, 2), flip(q, 3)
    core_peer, y_peer, diag_peer = (ep, q_core), (ep, q_y), (ep, q_diag)
    x_peer = (z * 2 + ox, q)

    def plane_peer(d):
        return (flip(z, d) * 2 + x, q)

    tok, width = tokens_ref.shape
    cap = tok // n_plane
    half = cap // 2
    inner = gate_hbm.shape[2]

    inputs = [
        pltpu.make_async_copy(source, target, load_sem.at[3 + i])
        for i, (source, target) in enumerate((
            (ids_hbm, ids_ref), (tokens_hbm, tokens_ref), (group_hbm, group_ref),
            (expert_hbm, expert_ref),
        ))
    ]
    for load in inputs:
        load.start()

    barrier = pltpu.get_barrier_semaphore()
    partners = [plane_peer(d) for d in range(1, n_plane)] + [x_peer, core_peer, y_peer, diag_peer]
    for peer in partners:
        pl.semaphore_signal(barrier, inc=1, device_id=peer, device_id_type=MESH)

    loads = [
        pltpu.make_async_copy(gate_hbm.at[0], w_in.at[:, pl.ds(0, inner)], load_sem.at[0]),
        pltpu.make_async_copy(up_hbm.at[0], w_in.at[:, pl.ds(inner, inner)], load_sem.at[1]),
        pltpu.make_async_copy(down_hbm.at[0], w_out, load_sem.at[2]),
    ]
    for load in loads:
        load.start()

    inputs[0].wait()
    first = ids_ref[0:1, :]
    group_row = (first >> 1).astype(F32)
    on_lanes = jnp.broadcast_to(group_row, (tok, tok))
    on_rows = jnp.transpose(on_lanes)
    ii = lax.broadcasted_iota(jnp.int32, (tok, tok), 0)
    jj = lax.broadcasted_iota(jnp.int32, (tok, tok), 1)
    same = on_lanes == on_rows
    zero, one = jnp.zeros((tok, tok), F32), jnp.ones((tok, tok), F32)
    rank_row = jnp.sum(jnp.where(same & (ii < jj), one, zero), axis=0, keepdims=True)
    rank_col = jnp.sum(jnp.where(same & (jj < ii), one, zero), axis=1, keepdims=True)
    place_row = group_row * cap + rank_row
    place_col = on_rows[:, 0:1] * cap + rank_col
    to_slot = jnp.broadcast_to(place_row, (tok, tok)) == ii.astype(F32)
    to_token = jnp.broadcast_to(place_col, (tok, tok)) == jj.astype(F32)

    inputs[1].wait()
    sorted_rows = jnp.dot(
        jnp.where(to_slot, one, zero).astype(BF16), tokens_ref[...], preferred_element_type=F32
    ).astype(BF16)
    outgoing[...] = sorted_rows.reshape(n_plane, cap, width)
    rows[q, x, z] = outgoing[z]

    inputs[2].wait()
    inputs[3].wait()
    weights = expert_ref[...]
    share = group_ref[...] * weights / jnp.sum(weights, axis=0, keepdims=True)
    even = (first & 1) == 0
    share_a = jnp.where(even, share[0:1, :], share[1:2, :])
    share_b = jnp.where(even, share[1:2, :], share[0:1, :])
    slot_a = jnp.sum(jnp.where(to_slot, jnp.broadcast_to(share_a, (tok, tok)), zero), axis=1, keepdims=True)
    slot_b = jnp.sum(jnp.where(to_slot, jnp.broadcast_to(share_b, (tok, tok)), zero), axis=1, keepdims=True)
    lane = lax.broadcasted_iota(jnp.int32, (tok, 128), 1)
    share_out[...] = jnp.where(lane < 64, slot_a, slot_b).reshape(n_plane, cap, 128)
    share_in[z] = share_out[z]

    pl.semaphore_wait(barrier, len(partners))

    started = []

    def copy(src, dst, kind, j, peer):
        return pltpu.make_async_remote_copy(
            src_ref=src, dst_ref=dst, send_sem=send_sem.at[kind, j], recv_sem=recv_sem.at[kind, j],
            device_id=peer, device_id_type=MESH,
        )

    def send(src, dst, kind, j, peer):
        c = copy(src, dst, kind, j, peer)
        c.start()
        started.append(c)

    def arrived(dst, kind, j):
        copy(dst, dst, kind, j, core_peer).wait_recv()

    low, high = pl.ds(0, half), pl.ds(half, half)
    for d in range(1, n_plane):
        for part, kind in ((low, TO_PLANE), (high, TO_PLANE_2)):
            send(outgoing.at[flip(z, d), part], rows.at[q, x, z, part], kind, d, plane_peer(d))

    def spread_own(j):
        block = rows.at[q, x, flip(z, j)]
        if j:
            arrived(block.at[low], TO_PLANE, j)
        send(block.at[low], block.at[low], ACROSS_X, j, x_peer)
        if j:
            send(block.at[low], block.at[low], ACROSS_Y2, j, y_peer)
            arrived(block.at[high], TO_PLANE_2, j)
        send(block.at[high], block.at[high], ACROSS_Y, j, y_peer)
        send(block.at[high], block.at[high], ACROSS_X2, j, x_peer)
        if not j:
            send(block.at[low], block.at[low], ACROSS_Y2, j, y_peer)
        send(block, block, CORE_OWN, j, core_peer)

    def pass_on(j):
        zz = flip(z, j)
        over_x, over_y = rows.at[q, ox, zz], rows.at[q_y, x, zz]
        arrived(over_x.at[low], ACROSS_X, j)
        send(over_x.at[low], over_x.at[low], RELAY_Y, j, y_peer)
        arrived(over_y.at[high], ACROSS_Y, j)
        send(over_y.at[high], over_y.at[high], RELAY_X, j, x_peer)
        arrived(over_x.at[high], ACROSS_X2, j)
        send(over_x, over_x, CORE_X, j, core_peer)
        arrived(over_y.at[low], ACROSS_Y2, j)
        send(over_y, over_y, CORE_Y, j, core_peer)

    def pass_relayed(j):
        block = rows.at[q_y, ox, flip(z, j)]
        arrived(block.at[low], RELAY_Y, j)
        send(block.at[low], block.at[low], CORE_RY, j, core_peer)
        arrived(block.at[high], RELAY_X, j)
        send(block.at[high], block.at[high], CORE_RX, j, core_peer)

    for step in range(n_plane + 1):
        if step < n_plane:
            spread_own(step)
        if step >= 1:
            pass_on(step - 1)
        if step >= 2:
            pass_relayed(step - 2)

    for d in range(1, n_plane):
        send(share_out.at[flip(z, d)], share_in.at[z], SHARES, d, plane_peer(d))

    def sums_of(column, quarter):
        part = rows[quarter, column].reshape(tok, width)
        w = w_in[pl.ds(pl.multiple_of(quarter * width, width), width), :]
        return jnp.dot(part, w, preferred_element_type=F32)

    def finish_hidden(total, column, kind):
        gate, up = total[:, :inner], total[:, inner:]
        hidden[column, q] = (gate / (1.0 + jnp.exp(-gate)) * up).astype(BF16)
        block = hidden.at[column, q]
        for d, peer in ((2, y_peer), (3, diag_peer), (1, core_peer)):
            send(block, block, kind, d, peer)

    def project(column, kind):
        for d in range(1, n_tp):
            arrived(hidden.at[column, flip(q, d)], kind, d)
        h = jnp.concatenate([hidden[column, t] for t in range(n_tp)], axis=1)
        return jnp.dot(h, w_out[...], preferred_element_type=F32).astype(BF16)

    loads[0].wait()
    loads[1].wait()
    total = sums_of(x, q) + sums_of(x, q_y)
    other = sums_of(ox, q)
    for j in range(n_plane):
        arrived(rows.at[q_core, x, flip(z, j)], CORE_OWN, j)
        arrived(rows.at[q_diag, x, flip(z, j)], CORE_Y, j)
    total = total + sums_of(x, q_core) + sums_of(x, q_diag)
    finish_hidden(total, x, HIDDEN_0)
    pass_relayed(n_plane - 1)
    for j in range(n_plane):
        arrived(rows.at[q_core, ox, flip(z, j)], CORE_X, j)
    other = other + sums_of(ox, q_core) + sums_of(ox, q_y)
    for j in range(n_plane):
        block = rows.at[q_diag, ox, flip(z, j)]
        arrived(block.at[low], CORE_RY, j)
        arrived(block.at[high], CORE_RX, j)
    other = other + sums_of(ox, q_diag)
    finish_hidden(other, ox, HIDDEN_1)

    loads[2].wait()
    for d in range(1, n_plane):
        arrived(share_in.at[flip(z, d)], SHARES, d)
    shares = share_in[...].reshape(tok, 128)
    is_first = x == 0
    share_own = jnp.where(is_first, shares[:, 0:1], shares[:, 64:65])
    share_other = jnp.where(is_first, shares[:, 64:65], shares[:, 0:1])
    own_part[...] = (project(x, HIDDEN_0).astype(F32) * share_own).reshape(n_plane, cap, width)
    share_in[...] = jnp.broadcast_to(share_other, (tok, 128)).reshape(n_plane, cap, 128)

    result_out[...] = project(ox, HIDDEN_1).reshape(n_plane, cap, width)
    order = tuple(range(n_plane - 1, -1, -1))
    pieces = ((low, 0, RESULT, BACK), (high, half, RESULT_2, BACK_2))
    for j in order:
        zz = flip(z, j)
        for part, _, there, _ in pieces:
            send(result_out.at[zz, part], result_in.at[zz, part], there, j, x_peer)
    for j in order:
        zz = flip(z, j)
        for part, at, there, home in pieces:
            arrived(result_in.at[zz, part], there, j)
            scaled = result_in[zz, at:at + half].astype(F32) * share_in[zz, at:at + half][:, 0:1]
            mixed_rows = (own_part[zz, at:at + half] + scaled).astype(BF16)
            if j:
                back_out[zz, at:at + half] = mixed_rows
                send(back_out.at[zz, part], back_in.at[z, part], home, j, plane_peer(j))
            else:
                back_in[z, at:at + half] = mixed_rows
    for j in order:
        if j:
            for part, _, _, home in pieces:
                arrived(back_in.at[flip(z, j), part], home, j)
    routed = jnp.dot(
        jnp.where(to_token, one, zero).astype(BF16),
        back_in[...].reshape(tok, width),
        preferred_element_type=F32,
    )
    mixed = residual_scale * tokens_ref[...].astype(F32) + routed
    mixed_ref[...] = mixed
    keep = pltpu.make_async_copy(mixed_ref, mixed_out, load_sem.at[7])
    keep.start()
    total_col = jnp.sum(mixed, axis=1, keepdims=True)
    centered = mixed - total_col / width
    square_col = jnp.sum(centered * centered, axis=1, keepdims=True)
    lane = lax.broadcasted_iota(jnp.int32, (tok, 128), 1)
    stats[q] = jnp.transpose(jnp.where(lane == 0, total_col, square_col))[0:8, :]
    for d, peer in ((3, diag_peer), (2, y_peer), (1, core_peer)):
        send(stats.at[q], stats.at[q], STATS, d, peer)
    for d in range(1, n_tp):
        arrived(stats.at[flip(q, d)], STATS, d)
    pieces = [stats[t] for t in range(n_tp)]
    full = width * n_tp
    center = sum(p[0:1, :] for p in pieces) / full
    spread = sum(p[1:2, :] + width * jnp.square(p[0:1, :] / width - center) for p in pieces) / full
    scale = lax.rsqrt(spread + norm_eps)
    sub = lax.broadcasted_iota(jnp.int32, (128, tok), 0)
    columns_out[...] = jnp.transpose(jnp.where(sub == 0, center, scale))
    keep.wait()
    for c in started:
        c.wait_send()


def norm_kernel(mixed_ref, columns_ref, gain_ref, bias_ref, out_ref):
    center, scale = columns_ref[:, 0:1], columns_ref[:, 1:2]
    out_ref[...] = (
        (mixed_ref[...] - center) * scale * gain_ref[...] + bias_ref[...]
    ).astype(BF16)


def pair_groups(
    tokens, expert_ids, group_weight, expert_weight, w_gate, w_up, w_down, norm_gain, norm_bias
):
    tok, width = tokens.shape
    n_plane = lax.axis_size("ep") // TOP_K
    n_tp = lax.axis_size("tp")
    cap = tok // n_plane
    inner = w_gate.shape[2]
    vmem = pl.BlockSpec(memory_space=pltpu.VMEM)
    hbm = pl.BlockSpec(memory_space=pltpu.HBM)
    mixed, columns = pl.pallas_call(
        functools.partial(layer_kernel, n_plane, n_tp),
        out_shape=(
            jax.ShapeDtypeStruct((tok, width), F32), jax.ShapeDtypeStruct((tok, 128), F32)
        ),
        in_specs=[hbm] * 7,
        out_specs=(pl.BlockSpec(memory_space=pl.ANY), vmem),
        scratch_shapes=[
            pltpu.VMEM((tok, width), BF16),
            pltpu.VMEM((TOP_K, tok), jnp.int32),
            pltpu.VMEM((1, tok), F32),
            pltpu.VMEM((TOP_K, tok), F32),
            pltpu.VMEM((tok, width), F32),
            pltpu.VMEM((w_gate.shape[1], 2 * inner), BF16),
            pltpu.VMEM(w_down.shape[1:], BF16),
            pltpu.VMEM((n_plane, cap, width), BF16),
            pltpu.VMEM((n_plane, cap, 128), F32),
            pltpu.VMEM((n_plane, cap, 128), F32),
            pltpu.VMEM((n_tp, 2, n_plane, cap, width), BF16),
            pltpu.VMEM((2, n_tp, tok, inner), BF16),
            pltpu.VMEM((n_plane, cap, width), F32),
            pltpu.VMEM((n_plane, cap, width), BF16),
            pltpu.VMEM((n_plane, cap, width), BF16),
            pltpu.VMEM((n_plane, cap, width), BF16),
            pltpu.VMEM((n_plane, cap, width), BF16),
            pltpu.VMEM((n_tp, 8, tok), F32),
            pltpu.SemaphoreType.DMA((KINDS, 4)),
            pltpu.SemaphoreType.DMA((KINDS, 4)),
            pltpu.SemaphoreType.DMA((8,)),
        ],
        compiler_params=pltpu.CompilerParams(
            collective_id=0, has_side_effects=True, vmem_limit_bytes=53 * 2**20
        ),
        name="layer",
    )(
        *(
            pltpu.with_memory_space_constraint(a, pltpu.HBM)
            for a in (
                tokens, expert_ids.T, group_weight[None, :], expert_weight.T, w_gate, w_up, w_down
            )
        )
    )
    return pl.pallas_call(
        norm_kernel,
        out_shape=jax.ShapeDtypeStruct((tok, width), BF16),
        in_specs=[vmem] * 4,
        out_specs=vmem,
        compiler_params=pltpu.CompilerParams(vmem_limit_bytes=8 * 2**20),
        name="norm",
    )(mixed, columns, norm_gain[None, :], norm_bias[None, :])


def solution(mesh):
    n_ep, n_tp = mesh.shape["ep"], mesh.shape["tp"]
    pairs = TOP_K == 2 and n_ep == GROUPS * TOP_K and n_tp == 4
    return jax.shard_map(
        pair_groups if pairs else on_device,
        mesh=mesh,
        in_specs=(
            P("ep", "tp"),
            P("ep", None),
            P("ep"),
            P("ep", None),
            P("ep", None, "tp"),
            P("ep", None, "tp"),
            P("ep", None, "tp"),
            P("tp"),
            P("tp"),
        ),
        out_specs=P("ep", "tp"),
        check_vma=False,
    )
```
